256 devices in a mesh: grp: 2 (over y), sp: 32 (over z, core), tp: 4 (over x).
Axes of the slice: x: 4, y: 2, z: 16, core: 2. Of those that a mesh axis runs over, the one named last changes fastest.
The devices are a block of a 4x16x16 slice.
Arguments:
- residual_in: bfloat16 [32768, 2048], P(('grp', 'sp', 'tp')), parts along dimension 0, may hold values from -6 to 6
- out_gate: bfloat16 [32768, 1024], P(('grp', 'sp', 'tp')), parts along dimension 0, may hold values from -6 to 6
- in_gate: bfloat16 [32768, 1024], P(('grp', 'sp', 'tp')), parts along dimension 0, may hold values from -6 to 6
- conv_input: bfloat16 [32768, 1024], P(('grp', 'sp', 'tp')), parts along dimension 0, may hold values from -6 to 6
- conv_kernel: bfloat16 [3, 1024], replicated, may hold values from -3.5 to 3.5
- mix_out: bfloat16 [1024, 2048], replicated, may hold values from -0.1875 to 0.1875
- post_mix_gain: float32 [2048], replicated, may hold values from 0.1 to 1.9
- pre_expert_gain: float32 [2048], replicated, may hold values from 0.1 to 1.9
- post_expert_gain: float32 [2048], replicated, may hold values from 0.1 to 1.9
- expert_ids: int32 [32768, 2], P(('grp', 'sp', 'tp')), parts along dimension 0, may hold values from 0 to 31, all different within a row; in each aligned block of 128 rows (0 to 127, 128 to 255, ...) at most 9 rows name the same one
- expert_weights: float32 [32768, 2], P(('grp', 'sp', 'tp')), parts along dimension 0, may hold values from 0.1 to 1
- gate_proj: bfloat16 [32, 2048, 2048], P('sp', None, 'tp'), may hold values from -0.375 to 0.375
- up_proj: bfloat16 [32, 2048, 2048], P('sp', None, 'tp'), may hold values from -0.375 to 0.375
- down_proj: bfloat16 [32, 2048, 2048], P('sp', 'tp'), may hold values from -0.125 to 0.125
Outputs:
- layer_out: bfloat16 [32768, 2048], P(('grp', 'sp', 'tp')), parts along dimension 0
The draws below stay inside these ranges and needn't reach their ends.
There are 2 independent parts, one for each index of `grp`. The reference program is written for one: setup_inputs(seed, part) draws one part's arguments, and reference() takes and returns one part's arrays. A program takes and returns all parts, laid end to end along the dimension named above; an argument that names none is the same for every part. Nothing has to cross between parts.
Inputs may be any that keep to these rules, and one draw needn't show every extreme that they name: `expert_ids`: each row names 2 different experts. Among the 128 rows of one device no expert is named by more than 9 rows, a bound that some block reaches of them.
All inputs are finite; a program needn't handle non-finite values.
Results may differ from the reference program's by a relative error of at most 0.0095.
Values may be sent and summed in bfloat16 or wider, within the bound.
No kernel may reach another device: no remote copies, remote signals or barrier semaphores. Data moves between devices by JAX's collectives and lax.ppermute only.
A program may use at most 64 MiB of HBM per device.

```python
import math
import jax
import jax.numpy as jnp
import numpy as np
from jax import lax

D = 2048
CONV_W = 1024
FF = 2048
TAPS = 3
TOP = 2
TOK_DEV = 128
TOKENS = 16384
EXPERTS = 32
CAP = 9
N_SP = 32
N_TP = 4


def steps_of(stream_key, extent, cuts, least, largest):
    factor_of, own = 1.0, jax.random.fold_in(stream_key, 6)
    for position, shards_of in cuts:
        draws = jnp.exp(jax.random.uniform(jax.random.fold_in(own, position), (shards_of,), jnp.float32, least / len(cuts), largest / len(cuts)))
        factor_of = factor_of * jnp.repeat(draws, extent[position] // shards_of).reshape([-1 if axis == position else 1 for axis in range(len(extent))])
    return factor_of


def shared_out(stream_key, own, number, rows, number_of, top, most, lean):
    ranking = jax.random.permutation(stream_key, number_of)
    heavy_load, common = shares(number_of, rows * top, most, lean, True), shares(number_of, rows * top, most, lean, False)
    places = jnp.arange(number_of)

    def named(lengths, offset_by):
        used = int((lengths > 0).sum())
        fixed = max(1, used // 4)
        passed = fixed + (places - fixed + offset_by * (used - fixed)) % max(1, number_of - fixed)
        return jnp.zeros((number_of,), jnp.int32).at[ranking[jnp.where(places < fixed, places, passed)]].set(jnp.asarray(lengths, jnp.int32))

    lengths = jnp.where(number % 4 == 0, named(heavy_load, number // 4), named(common, number - number // 4 - 1))
    mixed = jax.random.permutation(jax.random.fold_in(own, 3), number_of)
    giver, taker = mixed[0:number_of // 2 * 2:2], mixed[1:number_of // 2 * 2:2]
    margin = jnp.minimum(lengths[giver] - 1, most - lengths[taker]) // 2
    margin = jnp.where((giver == ranking[0]) | (taker == ranking[0]) | (lengths[taker] == 0), 0, jnp.maximum(margin, 0))
    passed = jax.random.randint(jax.random.fold_in(own, 4), (number_of // 2,), 0, 1 << 20) % (margin + 1)
    lengths = lengths.at[giver].add(-passed).at[taker].add(passed)
    labels = jnp.searchsorted(jnp.cumsum(lengths), jnp.arange(rows * top), side="right").astype(jnp.int32)
    listing = labels.reshape(top, rows).T
    listing = listing[jax.random.permutation(jax.random.fold_in(own, 1), rows)]
    offset_by = jax.random.randint(jax.random.fold_in(own, 2), (rows, 1), 0, top)
    return jnp.take_along_axis(listing, (jnp.arange(top)[None, :] + offset_by) % top, axis=1)


def shares(amount, total, most, skew, full):
    loads = [(1 << 20) // math.isqrt(grade ** skew) + 1 for grade in range(1, amount + 1)]
    largest = most if full else min(most, max(-(-total // amount), total * loads[0] // sum(loads)))
    least = 1 if total - largest >= amount - 1 else 0
    holding, rest = [largest] + [least] * (amount - 1), total - largest - least * (amount - 1)
    while rest > 0:
        free = [i for i in range(1, amount) if holding[i] < largest] or [i for i in range(1, amount) if holding[i] < most]
        mass, remaining = sum([loads[i] for i in free]), rest
        for i in free:
            extra = min(most - holding[i], max(1, remaining * loads[i] // mass), rest)
            holding[i] = holding[i] + extra
            rest = rest - extra
    return np.array(holding)


def normal_values(key, shape, scale, limit, split=(), kind=jnp.bfloat16):
    loudness = steps_of(key, shape, split, -0.22, 0.18) if split else 1.0
    entries = jax.random.normal(key, shape, jnp.float32) * scale * loudness
    return jnp.minimum(jnp.maximum(entries, -limit), limit).astype(kind)


def setup_inputs(seed: int = 0, part: int = 0) -> dict:
    arg_keys = jax.random.split(jax.random.key(seed), 15)
    part_keys = jax.random.split(jax.random.fold_in(arg_keys[14], part), 15)
    residual_in = normal_values(part_keys[0], (TOKENS, D), 1.0, 6.0, ((0, 128),))
    out_gate = normal_values(part_keys[1], (TOKENS, CONV_W), 1.0, 6.0, ((0, 128),))
    in_gate = normal_values(part_keys[2], (TOKENS, CONV_W), 1.0, 6.0, ((0, 128),))
    conv_input = normal_values(part_keys[3], (TOKENS, CONV_W), 1.0, 6.0, ((0, 128),))
    conv_kernel = normal_values(arg_keys[4], (TAPS, CONV_W), TAPS ** -0.5, 3.5)
    mix_out = normal_values(arg_keys[5], (CONV_W, D), CONV_W ** -0.5, 0.1875)
    post_mix_gain = jnp.clip(1.0 + 0.18 * jax.random.normal(arg_keys[6], (D,), jnp.float32), 0.1, 1.9)
    pre_expert_gain = jnp.clip(1.0 + 0.18 * jax.random.normal(arg_keys[7], (D,), jnp.float32), 0.1, 1.9)
    post_expert_gain = jnp.clip(1.0 + 0.18 * jax.random.normal(arg_keys[8], (D,), jnp.float32), 0.1, 1.9)
    expert_ids_keys = jax.random.split(jax.random.fold_in(part_keys[9], 1), TOKENS // TOK_DEV)
    expert_ids_turns = jax.random.permutation(jax.random.fold_in(part_keys[9], 3), TOKENS // TOK_DEV)
    expert_ids = jax.vmap(lambda own, number: shared_out(jax.random.fold_in(part_keys[9], 2), own, number, TOK_DEV, EXPERTS, TOP, CAP, 0))(expert_ids_keys, expert_ids_turns).reshape((TOKENS, TOP))
    expert_weights = jnp.clip(jnp.exp(math.log(1.0) - 2.3025851 * jax.random.uniform(part_keys[10], (TOKENS, TOP), jnp.float32) ** steps_of(part_keys[10], (TOKENS, TOP), ((0, 128),), -0.2, 0.2)), 0.1, 1.0)
    gate_proj = normal_values(arg_keys[11], (EXPERTS, D, FF), (D // 9) ** -0.5, 0.375, ((0, 32), (2, 4)))
    up_proj = normal_values(arg_keys[12], (EXPERTS, D, FF), (D // 9) ** -0.5, 0.375, ((0, 32), (2, 4)))
    down_proj = normal_values(arg_keys[13], (EXPERTS, FF, D), FF ** -0.5, 0.125, ((0, 32), (1, 4)))
    return dict(residual_in=residual_in, out_gate=out_gate, in_gate=in_gate, conv_input=conv_input, conv_kernel=conv_kernel, mix_out=mix_out, post_mix_gain=post_mix_gain, pre_expert_gain=pre_expert_gain, post_expert_gain=post_expert_gain, expert_ids=expert_ids, expert_weights=expert_weights, gate_proj=gate_proj, up_proj=up_proj, down_proj=down_proj)


def scaled_norm(values, gain):
    return values * lax.rsqrt(lax.optimization_barrier(jnp.mean(values * values, axis=-1, keepdims=True)) + 1e-06) * gain

def slot_of(routes):
    flat = routes.reshape(-1)
    onehot = (flat[:, None] == jnp.arange(EXPERTS, dtype=jnp.int32)[None, :]).astype(jnp.int32)
    before = jnp.cumsum(onehot, axis=0) - onehot
    return lax.optimization_barrier(jnp.sum(before * onehot, axis=1)).astype(jnp.int32)

def run_expert(rows, gate_w, up_w, down_w):
    gate = jnp.dot(rows, gate_w, preferred_element_type=jnp.float32)
    upper = jnp.dot(rows, up_w, preferred_element_type=jnp.float32)
    gate = jnp.minimum(gate, 7.0)
    upper = jnp.clip(upper, -7.0, 7.0)
    act = (gate * jax.nn.sigmoid(1.702 * gate) * (upper + 1.0)).astype(jnp.bfloat16)
    count = rows.shape[0]
    blocks = act.reshape(count, N_TP, FF // N_TP).astype(jnp.float32)
    down_blocks = down_w.reshape(N_TP, FF // N_TP, D).astype(jnp.float32)
    partial_value = jnp.einsum('npf,pfd->pnd', blocks, down_blocks).astype(jnp.bfloat16)
    return lax.optimization_barrier(jnp.sum(partial_value.astype(jnp.float32), axis=0)).astype(jnp.bfloat16)

def reference(residual_in, out_gate, in_gate, conv_input, conv_kernel, mix_out, post_mix_gain, pre_expert_gain, post_expert_gain, expert_ids, expert_weights, gate_proj, up_proj, down_proj):
    inputs = in_gate.astype(jnp.float32) * conv_input.astype(jnp.float32)
    padded = jnp.concatenate([jnp.zeros((2, CONV_W), jnp.float32), inputs], axis=0)
    taps = conv_kernel.astype(jnp.float32)
    conv = taps[0] * padded[:-2] + taps[1] * padded[1:-1] + taps[2] * padded[2:]
    mixed = (out_gate.astype(jnp.float32) * conv).astype(jnp.bfloat16)
    proj = jnp.dot(mixed, mix_out, preferred_element_type=jnp.float32)
    stream = (residual_in.astype(jnp.float32) + scaled_norm(proj, post_mix_gain)).astype(jnp.bfloat16)
    normed = scaled_norm(stream.astype(jnp.float32), pre_expert_gain).astype(jnp.bfloat16)
    sources = N_SP * N_TP
    routes = expert_ids.reshape(sources, TOK_DEV, TOP)
    slots = jax.vmap(slot_of)(routes)
    flat_e = routes.reshape(sources, TOK_DEV * TOP)
    source_ids = jnp.broadcast_to(jnp.arange(sources, dtype=jnp.int32)[:, None], flat_e.shape)
    token_ids = source_ids * TOK_DEV + (jnp.arange(TOK_DEV * TOP, dtype=jnp.int32) // TOP)[None, :]
    table = jnp.full((EXPERTS, sources, CAP), TOKENS, jnp.int32).at[flat_e, source_ids, slots].set(token_ids)
    weight_table = jnp.zeros((EXPERTS, sources, CAP), jnp.float32).at[flat_e, source_ids, slots].set(expert_weights.reshape(sources, TOK_DEV * TOP))
    padded_rows = jnp.concatenate([normed, jnp.zeros((1, D), jnp.bfloat16)], axis=0)

    def per_expert(total, item):
        index_rows, weight_rows, gate_w, up_w, down_w = item
        flat_index = index_rows.reshape(-1)
        output = run_expert(padded_rows[flat_index], gate_w, up_w, down_w)
        total = total.at[flat_index].add(output.astype(jnp.float32) * weight_rows.reshape(-1)[:, None])
        return (total, None)
    start = jnp.zeros((TOKENS + 1, D), jnp.float32)
    total, unused = lax.scan(per_expert, start, (table, weight_table, gate_proj, up_proj, down_proj))
    moe = total[:TOKENS]
    return (stream.astype(jnp.float32) + scaled_norm(moe, post_expert_gain)).astype(jnp.bfloat16)
```

```python
import jax
import jax.numpy as jnp
from jax import lax
from jax.sharding import Mesh
from jax.sharding import PartitionSpec as P


SP = ("sp_0", "sp_1")
SP_TP = ("sp_0", "sp_1", "tp")
GRP_SP_TP = ("grp", "sp_0", "sp_1", "tp")
LANES = 128
CHUNKS = 3


def from_behind(value, axis, steps):
    count = lax.axis_size(axis)
    initial, last = (max(0, -steps), min(count, count - steps))
    return lax.ppermute(value, axis, [(source, source + steps) for source in range(initial, last)])


def turned(value, axis, steps):
    count = lax.axis_size(axis)
    return lax.ppermute(value, axis, [(s, (s + steps) % count) for s in range(count)])


def scaled_norm(values, gain):
    return values * lax.rsqrt(jnp.mean(values * values, axis=-1, keepdims=True) + 1e-06) * gain


def body(
    residual_in,
    out_gate,
    in_gate,
    conv_input,
    conv_kernel,
    mix_out,
    post_mix_gain,
    pre_expert_gain,
    post_expert_gain,
    expert_ids,
    expert_weights,
    gate_proj,
    up_proj,
    down_proj,
):
    width = mix_out.shape[1]
    inputs = in_gate.astype(jnp.float32) * conv_input.astype(jnp.float32)
    prior = from_behind(inputs[-2:], SP_TP, 1)
    padded = jnp.concatenate([prior, inputs], axis=0)
    taps = conv_kernel.astype(jnp.float32)
    conv = taps[0] * padded[:-2] + taps[1] * padded[1:-1] + taps[2] * padded[2:]
    mixed = (out_gate.astype(jnp.float32) * conv).astype(jnp.bfloat16)
    proj = jnp.dot(mixed, mix_out, preferred_element_type=jnp.float32)
    stream = (residual_in.astype(jnp.float32) + scaled_norm(proj, post_mix_gain)).astype(
        jnp.bfloat16
    )
    normed = scaled_norm(stream.astype(jnp.float32), pre_expert_gain).astype(jnp.bfloat16)

    experts = lax.axis_size(SP)
    tp = lax.axis_size("tp")
    tok_rows = normed.shape[0]
    top = expert_ids.shape[1]
    mean_rows = tok_rows * top // experts
    capacity = max(2, mean_rows + max(1, tok_rows * top // (16 * experts)))
    step = capacity // CHUNKS
    rows = experts * step
    every = jnp.arange(experts, dtype=jnp.int32)
    token = jnp.arange(tok_rows, dtype=jnp.int32)
    named = expert_ids[:, :, None] == every
    member = named.any(axis=1)
    earlier = (token[:, None] > token[None, :]).astype(jnp.bfloat16)
    slot = jnp.dot(earlier, member.astype(jnp.bfloat16), preferred_element_type=jnp.float32)
    slot = jnp.where(member, slot, -1.0)
    slot_t = slot.T

    gate_w = gate_proj[0]
    up_w = up_proj[0]
    down_w = down_proj[0]

    def outbox(chunk):
        lanes = jnp.arange(step, dtype=jnp.float32) + chunk * step
        pick = (slot_t[:, None, :] == lanes[None, :, None]).astype(jnp.bfloat16)
        sent = jnp.dot(pick.reshape(rows, tok_rows), normed, preferred_element_type=jnp.float32)
        return sent.astype(jnp.bfloat16).reshape(experts, step, -1, LANES)

    def expert_rows(pieces):
        block = jnp.concatenate([p.reshape(rows, width) for p in pieces], axis=0)
        gate = jnp.dot(block, gate_w, preferred_element_type=jnp.float32)
        upper = jnp.dot(block, up_w, preferred_element_type=jnp.float32)
        gate = jnp.minimum(gate, 7.0)
        upper = jnp.clip(upper, -7.0, 7.0)
        act = (gate * jax.nn.sigmoid(1.702 * gate) * (upper + 1.0)).astype(jnp.bfloat16)
        made = jnp.dot(act, down_w, preferred_element_type=jnp.float32).astype(jnp.bfloat16)
        return made.reshape(tp, rows, -1, LANES)

    def exchanged(blocks):
        return lax.all_to_all(blocks, SP, split_axis=0, concat_axis=0, tiled=True)

    back = []
    for chunk in range(CHUNKS):
        here = exchanged(outbox(chunk)).reshape(rows, -1, LANES)
        pieces = [here] + [turned(here, "tp", d) for d in range(1, tp)]
        made = expert_rows(pieces)
        sums = made[0].astype(jnp.float32)
        for d in range(1, tp):
            sums = sums + turned(made[d], "tp", -d).astype(jnp.float32)
        summed = sums.astype(jnp.bfloat16).reshape(experts, step, -1, LANES)
        back.append(exchanged(summed).reshape(rows, width))

    moe = 0.0
    for k in range(top):
        found = 0.0
        for chunk in range(CHUNKS):
            lanes = jnp.arange(step, dtype=jnp.float32) + chunk * step
            pick = (jnp.where(named[:, k], slot, -1.0)[:, :, None] == lanes).astype(jnp.bfloat16)
            found = found + jnp.dot(
                pick.reshape(tok_rows, rows), back[chunk], preferred_element_type=jnp.float32
            )
        moe = moe + found * expert_weights[:, k : k + 1]
    return (stream.astype(jnp.float32) + scaled_norm(moe, post_expert_gain)).astype(jnp.bfloat16)


def solution(mesh):
    split = Mesh(
        mesh.devices.reshape(mesh.shape["grp"], -1, 2, mesh.shape["tp"]),
        GRP_SP_TP,
    )
    tokens = P(GRP_SP_TP, None)
    in_specs = (
        (tokens,) * 4
        + (P(),) * 5
        + (tokens, tokens, P(SP, None, "tp"), P(SP, None, "tp"), P(SP, "tp", None))
    )
    return jax.shard_map(body, mesh=split, in_specs=in_specs, out_specs=tokens, check_vma=False)
```

```python
import jax
import jax.numpy as jnp
from jax import lax
from jax.experimental import pallas as pl
from jax.experimental.pallas import tpu as pltpu
from jax.sharding import Mesh
from jax.sharding import PartitionSpec as P


SP = ("sp_0", "sp_1")
SP_TP = ("sp_0", "sp_1", "tp")
GRP_SP_TP = ("grp", "sp_0", "sp_1", "tp")
LANES = 128
CHUNKS = 3


def from_behind(value, axis, steps):
    count = lax.axis_size(axis)
    initial, last = (max(0, -steps), min(count, count - steps))
    return lax.ppermute(value, axis, [(source, source + steps) for source in range(initial, last)])


def turned(value, axis, steps):
    count = lax.axis_size(axis)
    return lax.ppermute(value, axis, [(s, (s + steps) % count) for s in range(count)])


def scaled_norm(values, gain):
    return values * lax.rsqrt(jnp.mean(values * values, axis=-1, keepdims=True) + 1e-06) * gain


def expert_kernel(count, *refs):
    pieces, (gate_ref, up_ref, down_ref) = refs[:count], refs[count : count + 3]
    outs = refs[count + 3 : 2 * count + 3]
    wide, flat, act_ref = refs[2 * count + 3 :]
    rows, sub, lanes = pieces[0].shape
    total = count * rows
    for i, piece in enumerate(pieces):
        wide[pl.ds(i * rows * sub, rows * sub), :] = (
            piece[...].reshape(rows * sub, lanes).astype(jnp.float32)
        )
    for s in range(sub):
        flat[:, s * lanes : (s + 1) * lanes] = wide[pl.ds(s, total, stride=sub), :].astype(
            jnp.bfloat16
        )
    hidden = act_ref.shape[1]
    block = 256
    for h in range(0, hidden, block):
        x = flat[...]
        gate = jnp.dot(x, gate_ref[:, h : h + block], preferred_element_type=jnp.float32)
        upper = jnp.dot(x, up_ref[:, h : h + block], preferred_element_type=jnp.float32)
        gate = jnp.minimum(gate, 7.0)
        upper = jnp.clip(upper, -7.0, 7.0)
        act = gate * jax.nn.sigmoid(1.702 * gate) * (upper + 1.0)
        act_ref[:, h : h + block] = act.astype(jnp.bfloat16)
    for s in range(0, sub, block // lanes):
        made = jnp.dot(
            act_ref[...],
            down_ref[:, s * lanes : s * lanes + block],
            preferred_element_type=jnp.float32,
        )
        for t in range(block // lanes):
            wide[pl.ds(s + t, total, stride=sub), :] = made[:, t * lanes : (t + 1) * lanes]
    for i, out in enumerate(outs):
        part = wide[pl.ds(i * rows * sub, rows * sub), :]
        out[...] = part.astype(jnp.bfloat16).reshape(rows, sub, lanes)


def expert_rows(pieces, gate_w, up_w, down_w):
    count = len(pieces)
    rows, sub, lanes = pieces[0].shape
    total = count * rows
    spec = pl.BlockSpec(memory_space=pltpu.VMEM)
    return pl.pallas_call(
        lambda *refs: expert_kernel(count, *refs),
        in_specs=[spec] * (count + 3),
        out_specs=[spec] * count,
        out_shape=[jax.ShapeDtypeStruct(p.shape, p.dtype) for p in pieces],
        scratch_shapes=[
            pltpu.VMEM((total * sub, lanes), jnp.float32),
            pltpu.VMEM((total, sub * lanes), jnp.bfloat16),
            pltpu.VMEM((total, gate_w.shape[1]), jnp.bfloat16),
        ],
        compiler_params=pltpu.CompilerParams(vmem_limit_bytes=48 << 20),
        name="experts",
    )(*pieces, gate_w, up_w, down_w)


def body(
    residual_in,
    out_gate,
    in_gate,
    conv_input,
    conv_kernel,
    mix_out,
    post_mix_gain,
    pre_expert_gain,
    post_expert_gain,
    expert_ids,
    expert_weights,
    gate_proj,
    up_proj,
    down_proj,
):
    width = mix_out.shape[1]
    inputs = in_gate.astype(jnp.float32) * conv_input.astype(jnp.float32)
    prior = from_behind(inputs[-2:], SP_TP, 1)
    padded = jnp.concatenate([prior, inputs], axis=0)
    taps = conv_kernel.astype(jnp.float32)
    conv = taps[0] * padded[:-2] + taps[1] * padded[1:-1] + taps[2] * padded[2:]
    mixed = (out_gate.astype(jnp.float32) * conv).astype(jnp.bfloat16)
    proj = jnp.dot(mixed, mix_out, preferred_element_type=jnp.float32)
    stream = (residual_in.astype(jnp.float32) + scaled_norm(proj, post_mix_gain)).astype(
        jnp.bfloat16
    )
    normed = scaled_norm(stream.astype(jnp.float32), pre_expert_gain).astype(jnp.bfloat16)

    experts = lax.axis_size(SP)
    places = lax.axis_size("sp_0")
    cores = lax.axis_size("sp_1")
    tp = lax.axis_size("tp")
    core = lax.axis_index("sp_1")
    tok_rows = normed.shape[0]
    top = expert_ids.shape[1]
    mean_rows = tok_rows * top // experts
    capacity = max(2, mean_rows + max(1, tok_rows * top // (16 * experts)))
    step = capacity // CHUNKS
    rows = places * step
    slots = jnp.arange(capacity, dtype=jnp.float32).reshape(CHUNKS, step)
    every = (
        jnp.arange(places, dtype=jnp.int32)[:, None] * cores
        + (jnp.arange(cores, dtype=jnp.int32)[None, :] + core) % cores
    ).reshape(-1)
    token = jnp.arange(tok_rows, dtype=jnp.int32)
    named = expert_ids[:, :, None] == every
    member = named.any(axis=1)
    earlier = (token[:, None] > token[None, :]).astype(jnp.bfloat16)
    slot = jnp.dot(earlier, member.astype(jnp.bfloat16), preferred_element_type=jnp.float32)
    slot_t = jnp.where(member, slot, -1.0).T

    def outbox(chunk):
        pick = (slot_t[:, None, :] == slots[chunk][None, :, None]).astype(jnp.bfloat16)
        sent = jnp.dot(
            pick.reshape(-1, tok_rows), normed, preferred_element_type=jnp.float32
        )
        return sent.astype(jnp.bfloat16).reshape(places, cores, step, -1, LANES)

    def exchanged(blocks):
        return lax.all_to_all(blocks, "sp_0", split_axis=0, concat_axis=0, tiled=True)

    def rowed(block):
        return block.reshape(rows, -1, LANES)

    back = []
    for chunk in range(CHUNKS):
        came = exchanged(outbox(chunk))
        other = turned(rowed(came[:, 1]), "sp_1", 1)
        here = jnp.concatenate([rowed(came[:, 0]), other], axis=0)
        pieces = [here] + [turned(here, "tp", d) for d in range(1, tp)]
        made = expert_rows(pieces, gate_proj[0], up_proj[0], down_proj[0])
        sums = made[0].astype(jnp.float32)
        for d in range(1, tp):
            sums = sums + turned(made[d], "tp", -d).astype(jnp.float32)
        summed = sums.astype(jnp.bfloat16)
        other = turned(summed[rows:], "sp_1", 1)
        ready = jnp.stack(
            [b.reshape(places, step, -1, LANES) for b in (summed[:rows], other)], axis=1
        )
        back.append(exchanged(ready).reshape(cores * rows, width))

    moe = 0.0
    for k in range(top):
        found = 0.0
        for chunk in range(CHUNKS):
            pick = jnp.where(named[:, k], slot, -1.0)[:, :, None] == slots[chunk]
            found = found + jnp.dot(
                pick.astype(jnp.bfloat16).reshape(tok_rows, -1),
                back[chunk],
                preferred_element_type=jnp.float32,
            )
        moe = moe + found * expert_weights[:, k : k + 1]
    return (stream.astype(jnp.float32) + scaled_norm(moe, post_expert_gain)).astype(jnp.bfloat16)


def solution(mesh):
    split = Mesh(
        mesh.devices.reshape(mesh.shape["grp"], -1, 2, mesh.shape["tp"]),
        GRP_SP_TP,
    )
    tokens = P(GRP_SP_TP, None)
    in_specs = (
        (tokens,) * 4
        + (P(),) * 5
        + (tokens, tokens, P(SP, None, "tp"), P(SP, None, "tp"), P(SP, "tp", None))
    )
    return jax.shard_map(body, mesh=split, in_specs=in_specs, out_specs=tokens, check_vma=False)
```

```python
import math

import jax
import jax.numpy as jnp
from jax import lax
from jax.experimental import pallas as pl
from jax.experimental.pallas import tpu as pltpu
from jax.sharding import Mesh
from jax.sharding import PartitionSpec as P


SP = ("sp_0", "sp_1")
SP_TP = ("sp_0", "sp_1", "tp")
GRP_SP_TP = ("grp", "sp_0", "sp_1", "tp")
LANES = 128
FIRST = 4


def from_behind(value, axis, steps):
    count = lax.axis_size(axis)
    initial, last = (max(0, -steps), min(count, count - steps))
    return lax.ppermute(value, axis, [(source, source + steps) for source in range(initial, last)])


def turned(value, axis, steps):
    count = lax.axis_size(axis)
    return lax.ppermute(value, axis, [(s, (s + steps) % count) for s in range(count)])


def scaled_norm(values, gain):
    return values * lax.rsqrt(jnp.mean(values * values, axis=-1, keepdims=True) + 1e-06) * gain


def expert_kernel(count, *refs):
    pieces, (gate_ref, up_ref, down_ref) = refs[:count], refs[count : count + 3]
    outs = refs[count + 3 : 2 * count + 3]
    wide, flat, act_ref = refs[2 * count + 3 :]
    rows, sub, lanes = pieces[0].shape
    total = count * rows
    for i, piece in enumerate(pieces):
        wide[pl.ds(i * rows * sub, rows * sub), :] = (
            piece[...].reshape(rows * sub, lanes).astype(jnp.float32)
        )
    for s in range(sub):
        flat[:, s * lanes : (s + 1) * lanes] = wide[pl.ds(s, total, stride=sub), :].astype(
            jnp.bfloat16
        )
    hidden = act_ref.shape[1]
    block = 256
    for h in range(0, hidden, block):
        x = flat[...]
        gate = jnp.dot(x, gate_ref[:, h : h + block], preferred_element_type=jnp.float32)
        upper = jnp.dot(x, up_ref[:, h : h + block], preferred_element_type=jnp.float32)
        gate = jnp.minimum(gate, 7.0)
        upper = jnp.clip(upper, -7.0, 7.0)
        act = gate * jax.nn.sigmoid(1.702 * gate) * (upper + 1.0)
        act_ref[:, h : h + block] = act.astype(jnp.bfloat16)
    for s in range(0, sub, block // lanes):
        made = jnp.dot(
            act_ref[...],
            down_ref[:, s * lanes : s * lanes + block],
            preferred_element_type=jnp.float32,
        )
        for t in range(block // lanes):
            wide[pl.ds(s + t, total, stride=sub), :] = made[:, t * lanes : (t + 1) * lanes]
    for i, out in enumerate(outs):
        part = wide[pl.ds(i * rows * sub, rows * sub), :]
        out[...] = part.astype(jnp.bfloat16).reshape(rows, sub, lanes)


def vmem_call(kernel, outs, args, scratch=()):
    spec = pl.BlockSpec(memory_space=pltpu.VMEM)
    return pl.pallas_call(
        kernel,
        in_specs=[spec] * len(args),
        out_specs=[spec] * len(outs),
        out_shape=outs,
        scratch_shapes=list(scratch),
        compiler_params=pltpu.CompilerParams(vmem_limit_bytes=48 << 20),
    )(*args)


def expert_rows(pieces, gate_w, up_w, down_w):
    count = len(pieces)
    rows, sub, lanes = pieces[0].shape
    total = count * rows
    return vmem_call(
        lambda *refs: expert_kernel(count, *refs),
        [jax.ShapeDtypeStruct(p.shape, p.dtype) for p in pieces],
        (*pieces, gate_w, up_w, down_w),
        (
            pltpu.VMEM((total * sub, lanes), jnp.float32),
            pltpu.VMEM((total, sub * lanes), jnp.bfloat16),
            pltpu.VMEM((total, gate_w.shape[1]), jnp.bfloat16),
        ),
    )


def ring_parts(places):
    quarter = places // 4
    parts = [(0, (0,))]
    for sign in (1, -1):
        for b in range(quarter - 1, 0, -1):
            parts.append((sign * b, (sign * b, sign * (quarter + b))))
    parts += [(quarter, (quarter,)), (-quarter, (-quarter,)), (2 * quarter, (2 * quarter,))]
    return parts


def ring_arrivals(places):
    quarter = places // 4
    found = []
    for shift, units in ring_parts(places):
        if abs(shift) == quarter:
            sign = shift // quarter
            units = tuple(sign * (quarter + b) for b in range(quarter))
        found.append(units if abs(shift) == quarter else units[:1])
    return found


def ring_exchange(arrays, axis):
    places = lax.axis_size(axis)
    quarter = places // 4
    moved = {}
    for (shift, units), array in zip(ring_parts(places), arrays):
        if abs(shift) < quarter or shift == 2 * quarter:
            moved[shift] = turned(array, axis, shift) if shift else array
    for (shift, units), array in zip(ring_parts(places), arrays):
        if abs(shift) == quarter:
            sign = shift // quarter
            joined = [array] + [moved[sign * b][1:] for b in range(1, quarter)]
            joined = jnp.concatenate(joined, axis=0)
            moved[shift] = turned(joined, axis, shift)
    return [moved[shift] for shift, _ in ring_parts(places)]


def outbox_kernel(pick_ref, normed_ref, *refs):
    outs, wide = refs[:-1], refs[-1]
    rows, lanes = pick_ref.shape[0], wide.shape[1]
    sub = wide.shape[0] // rows
    sent = jnp.dot(pick_ref[...], normed_ref[...], preferred_element_type=jnp.float32)
    for s in range(sub):
        wide[pl.ds(s, rows, stride=sub), :] = sent[:, s * lanes : (s + 1) * lanes]
    begin = 0
    for out in outs:
        size = math.prod(out.shape[:-2]) * sub
        out[...] = wide[pl.ds(begin, size), :].astype(out.dtype).reshape(out.shape)
        begin += size


def outbox(pick, normed, places, cores, step):
    width = normed.shape[1]
    outs = [
        jax.ShapeDtypeStruct((len(units), cores, step, width // LANES, LANES), normed.dtype)
        for _, units in ring_parts(places)
    ]
    scratch = (pltpu.VMEM((pick.shape[0] * width // LANES, LANES), jnp.float32),)
    return vmem_call(outbox_kernel, outs, (pick, normed), scratch)


def parted_kernel(places, *refs):
    keep, other = refs[-2:]
    step = refs[0].shape[2]
    place = 0
    for ref, units in zip(refs, ring_arrivals(places)):
        for k, _ in enumerate(units):
            keep[place * step : (place + 1) * step] = ref[k, 0]
            other[place * step : (place + 1) * step] = ref[k, 1]
            place += 1


def parted(arrays, places):
    shape = arrays[0].shape
    out = jax.ShapeDtypeStruct((places * shape[2], *shape[3:]), arrays[0].dtype)
    return vmem_call(lambda *refs: parted_kernel(places, *refs), [out, out], arrays, ())


def summed_kernel(own, first, second, third, keep, other):
    half = keep.shape[0]
    for out, begin in ((keep, 0), (other, half)):
        total = own[begin : begin + half].astype(jnp.float32)
        for ref in (first, second, third):
            total = total + ref[begin : begin + half].astype(jnp.float32)
        out[...] = total.astype(out.dtype)


def summed_parts(parts):
    shape = parts[0].shape
    out = jax.ShapeDtypeStruct((shape[0] // 2, *shape[1:]), parts[0].dtype)
    return vmem_call(summed_kernel, [out, out], parts, ())


def returned_kernel(places, keep, other, *outs):
    step = outs[0].shape[2]
    order = [unit for units in ring_arrivals(places) for unit in units]
    for out, (_, units) in zip(outs, ring_parts(places)):
        for k, unit in enumerate(units):
            place = order.index(-unit if 2 * abs(unit) < places else unit)
            out[k, 0] = keep[place * step : (place + 1) * step]
            out[k, 1] = other[place * step : (place + 1) * step]


def returned(keep, other, places, cores):
    step = keep.shape[0] // places
    outs = [
        jax.ShapeDtypeStruct((len(units), cores, step, *keep.shape[1:]), keep.dtype)
        for _, units in ring_parts(places)
    ]
    return vmem_call(lambda *refs: returned_kernel(places, *refs), outs, (keep, other), ())


def combine_kernel(places, *refs):
    arrays, (picks, weights, out, wide, flat) = refs[:-5], refs[-5:]
    sub, lanes = arrays[0].shape[-2:]
    begin = 0
    for ref, units in zip(arrays, ring_arrivals(places)):
        size = len(units) * ref.shape[1] * ref.shape[2] * sub
        part = ref[: len(units)].astype(jnp.float32)
        wide[pl.ds(begin, size), :] = part.reshape(size, lanes)
        begin += size
    rows = flat.shape[0]
    for s in range(sub):
        flat[:, s * lanes : (s + 1) * lanes] = wide[pl.ds(s, rows, stride=sub), :].astype(
            flat.dtype
        )
    block = 4 * lanes
    for s in range(0, flat.shape[1], block):
        total = 0.0
        for k in range(picks.shape[0]):
            found = jnp.dot(
                picks[k], flat[:, s : s + block], preferred_element_type=jnp.float32
            )
            total = total + found * weights[:, k : k + 1]
        out[:, s : s + block] = total


def combined(arrays, picks, weights, places):
    rows = picks.shape[2]
    sub, lanes = arrays[0].shape[-2:]
    return vmem_call(
        lambda *refs: combine_kernel(places, *refs),
        [jax.ShapeDtypeStruct((picks.shape[1], sub * lanes), jnp.float32)],
        (*arrays, picks, weights),
        (
            pltpu.VMEM((rows * sub, lanes), jnp.float32),
            pltpu.VMEM((rows, sub * lanes), jnp.bfloat16),
        ),
    )[0]


def body(
    residual_in,
    out_gate,
    in_gate,
    conv_input,
    conv_kernel,
    mix_out,
    post_mix_gain,
    pre_expert_gain,
    post_expert_gain,
    expert_ids,
    expert_weights,
    gate_proj,
    up_proj,
    down_proj,
):
    inputs = in_gate.astype(jnp.float32) * conv_input.astype(jnp.float32)
    prior = from_behind(inputs[-2:], SP_TP, 1)
    padded = jnp.concatenate([prior, inputs], axis=0)
    taps = conv_kernel.astype(jnp.float32)
    conv = taps[0] * padded[:-2] + taps[1] * padded[1:-1] + taps[2] * padded[2:]
    mixed = (out_gate.astype(jnp.float32) * conv).astype(jnp.bfloat16)
    proj = jnp.dot(mixed, mix_out, preferred_element_type=jnp.float32)
    stream = (residual_in.astype(jnp.float32) + scaled_norm(proj, post_mix_gain)).astype(
        jnp.bfloat16
    )
    normed = scaled_norm(stream.astype(jnp.float32), pre_expert_gain).astype(jnp.bfloat16)

    experts = lax.axis_size(SP)
    places = lax.axis_size("sp_0")
    cores = lax.axis_size("sp_1")
    tp = lax.axis_size("tp")
    core = lax.axis_index("sp_1")
    tok_rows = normed.shape[0]
    top = expert_ids.shape[1]
    mean_rows = tok_rows * top // experts
    capacity = max(2, mean_rows + max(1, tok_rows * top // (16 * experts)))
    place = lax.axis_index("sp_0")
    sizes = [FIRST, capacity - FIRST]
    begins = [0, FIRST]
    token = jnp.arange(tok_rows, dtype=jnp.int32)
    every = jnp.arange(experts, dtype=jnp.int32)
    named = expert_ids[:, :, None] == every
    member = named.any(axis=1)
    earlier = (token[:, None] > token[None, :]).astype(jnp.bfloat16)
    slot = jnp.dot(earlier, member.astype(jnp.bfloat16), preferred_element_type=jnp.float32)
    taken = jnp.sum(jnp.where(named, slot[:, None, :], 0.0), axis=2).astype(jnp.int32)

    def row_names(units, begin, step):
        away = jnp.array(units, jnp.int32)[:, None, None]
        turn = jnp.arange(cores, dtype=jnp.int32)[None, :, None]
        slots = jnp.arange(step, dtype=jnp.int32)[None, None, :] + begin
        expert = (place + away) % places * cores + (turn + core) % cores
        return (expert * capacity + slots).reshape(-1)

    code = expert_ids * capacity + taken
    parts = [unit for _, units in ring_parts(places) for unit in units]
    arrivals = [-unit for units in ring_arrivals(places) for unit in units]

    weights = (gate_proj[0], up_proj[0], down_proj[0])
    moe = 0.0
    for begin, step in zip(begins, sizes):
        rows = row_names(parts, begin, step)
        pick = (rows[:, None] == code[:, 0]) | (rows[:, None] == code[:, 1])
        sent = outbox(pick.astype(jnp.bfloat16), normed, places, cores, step)
        came = ring_exchange(sent, "sp_0")
        keep, other = parted(came, places)
        other = turned(other, "sp_1", 1)
        here = jnp.concatenate([keep, other], axis=0)
        pieces = [here] + [turned(here, "tp", d) for d in range(1, tp)]
        made = expert_rows(pieces, *weights)
        made = [made[0]] + [turned(made[d], "tp", -d) for d in range(1, tp)]
        keep, other = summed_parts(made)
        other = turned(other, "sp_1", 1)
        sent = returned(keep, other, places, cores)
        back = ring_exchange(sent, "sp_0")
        rows = row_names(arrivals, begin, step)
        picks = (code.T[:, :, None] == rows).astype(jnp.bfloat16)
        moe = moe + combined(back, picks, expert_weights, places)
    return (stream.astype(jnp.float32) + scaled_norm(moe, post_expert_gain)).astype(jnp.bfloat16)


def solution(mesh):
    split = Mesh(
        mesh.devices.reshape(mesh.shape["grp"], -1, 2, mesh.shape["tp"]),
        GRP_SP_TP,
    )
    tokens = P(GRP_SP_TP, None)
    in_specs = (
        (tokens,) * 4
        + (P(),) * 5
        + (tokens, tokens, P(SP, None, "tp"), P(SP, None, "tp"), P(SP, "tp", None))
    )
    return jax.shard_map(body, mesh=split, in_specs=in_specs, out_specs=tokens, check_vma=False)
```

```python
import jax
import jax.numpy as jnp
from jax import lax
from jax.experimental import pallas as pl
from jax.experimental.pallas import tpu as pltpu
from jax.sharding import Mesh
from jax.sharding import PartitionSpec as P


SP = ("sp_0", "sp_1")
SP_TP = ("sp_0", "sp_1", "tp")
GRP_SP_TP = ("grp", "sp_0", "sp_1", "tp")
LANES = 128
CHUNKS = 3


def from_behind(value, axis, steps):
    count = lax.axis_size(axis)
    initial, last = (max(0, -steps), min(count, count - steps))
    return lax.ppermute(value, axis, [(source, source + steps) for source in range(initial, last)])


def turned(value, axis, steps):
    count = lax.axis_size(axis)
    return lax.ppermute(value, axis, [(s, (s + steps) % count) for s in range(count)])


def scaled_norm(values, gain):
    return values * lax.rsqrt(jnp.mean(values * values, axis=-1, keepdims=True) + 1e-06) * gain


def expert_kernel(count, *refs):
    pieces, (gate_ref, up_ref, down_ref) = refs[:count], refs[count : count + 3]
    outs = refs[count + 3 : 2 * count + 3]
    wide, flat, act_ref = refs[2 * count + 3 :]
    rows, sub, lanes = pieces[0].shape
    total = count * rows
    few = 8
    block = 2 * lanes

    def widen(j, _):
        for i, piece in enumerate(pieces):
            at = pl.multiple_of((i * rows + j * few) * sub, few * sub)
            part = piece[pl.ds(j * few, few)].astype(jnp.float32)
            wide[pl.ds(at, few * sub), :] = part.reshape(few * sub, lanes)
        return 0

    def flatten(s, _):
        at = pl.multiple_of(s * lanes, lanes)
        flat[:, pl.ds(at, lanes)] = wide[pl.ds(s, total, stride=sub), :].astype(flat.dtype)
        return 0

    def activate(h, _):
        at = pl.ds(pl.multiple_of(h * block, block), block)
        gate = jnp.dot(flat[...], gate_ref[:, at], preferred_element_type=jnp.float32)
        upper = jnp.dot(flat[...], up_ref[:, at], preferred_element_type=jnp.float32)
        gate = jnp.minimum(gate, 7.0)
        upper = jnp.clip(upper, -7.0, 7.0)
        act = gate * jax.nn.sigmoid(1.702 * gate) * (upper + 1.0)
        act_ref[:, at] = act.astype(act_ref.dtype)
        return 0

    def project(h, _):
        at = pl.ds(pl.multiple_of(h * block, block), block)
        made = jnp.dot(act_ref[...], down_ref[:, at], preferred_element_type=jnp.float32)
        for t in range(2):
            wide[pl.ds(2 * h + t, total, stride=sub), :] = made[:, t * lanes : (t + 1) * lanes]
        return 0

    def narrow(j, _):
        for i, out in enumerate(outs):
            at = pl.multiple_of((i * rows + j * few) * sub, few * sub)
            part = wide[pl.ds(at, few * sub), :].astype(out.dtype)
            out[pl.ds(j * few, few)] = part.reshape(few, sub, lanes)
        return 0

    lax.fori_loop(0, rows // few, widen, 0)
    lax.fori_loop(0, sub, flatten, 0)
    lax.fori_loop(0, act_ref.shape[1] // block, activate, 0)
    lax.fori_loop(0, sub * lanes // block, project, 0)
    lax.fori_loop(0, rows // few, narrow, 0)


def expert_rows(pieces, gate_w, up_w, down_w):
    count = len(pieces)
    rows, sub, lanes = pieces[0].shape
    total = count * rows
    spec = pl.BlockSpec(memory_space=pltpu.VMEM)
    return pl.pallas_call(
        lambda *refs: expert_kernel(count, *refs),
        in_specs=[spec] * (count + 3),
        out_specs=[spec] * count,
        out_shape=[jax.ShapeDtypeStruct(p.shape, p.dtype) for p in pieces],
        scratch_shapes=[
            pltpu.VMEM((total * sub, lanes), jnp.float32),
            pltpu.VMEM((total, sub * lanes), jnp.bfloat16),
            pltpu.VMEM((total, gate_w.shape[1]), jnp.bfloat16),
        ],
        compiler_params=pltpu.CompilerParams(vmem_limit_bytes=48 << 20),
        name="experts",
    )(*pieces, gate_w, up_w, down_w)


def body(
    residual_in,
    out_gate,
    in_gate,
    conv_input,
    conv_kernel,
    mix_out,
    post_mix_gain,
    pre_expert_gain,
    post_expert_gain,
    expert_ids,
    expert_weights,
    gate_proj,
    up_proj,
    down_proj,
):
    width = mix_out.shape[1]
    inputs = in_gate.astype(jnp.float32) * conv_input.astype(jnp.float32)
    prior = from_behind(inputs[-2:], SP_TP, 1)
    padded = jnp.concatenate([prior, inputs], axis=0)
    taps = conv_kernel.astype(jnp.float32)
    conv = taps[0] * padded[:-2] + taps[1] * padded[1:-1] + taps[2] * padded[2:]
    mixed = (out_gate.astype(jnp.float32) * conv).astype(jnp.bfloat16)
    proj = jnp.dot(mixed, mix_out, preferred_element_type=jnp.float32)
    stream = (residual_in.astype(jnp.float32) + scaled_norm(proj, post_mix_gain)).astype(
        jnp.bfloat16
    )
    normed = scaled_norm(stream.astype(jnp.float32), pre_expert_gain).astype(jnp.bfloat16)

    experts = lax.axis_size(SP)
    places = lax.axis_size("sp_0")
    cores = lax.axis_size("sp_1")
    tp = lax.axis_size("tp")
    core = lax.axis_index("sp_1")
    tok_rows = normed.shape[0]
    top = expert_ids.shape[1]
    mean_rows = tok_rows * top // experts
    capacity = max(2, mean_rows + max(1, tok_rows * top // (16 * experts)))
    step = capacity // CHUNKS
    rows = places * step
    slots = jnp.arange(capacity, dtype=jnp.float32).reshape(CHUNKS, step)
    every = (
        jnp.arange(places, dtype=jnp.int32)[:, None] * cores
        + (jnp.arange(cores, dtype=jnp.int32)[None, :] + core) % cores
    ).reshape(-1)
    token = jnp.arange(tok_rows, dtype=jnp.int32)
    named = expert_ids[:, :, None] == every
    member = named.any(axis=1)
    earlier = (token[:, None] > token[None, :]).astype(jnp.bfloat16)
    slot = jnp.dot(earlier, member.astype(jnp.bfloat16), preferred_element_type=jnp.float32)
    slot_t = jnp.where(member, slot, -1.0).T

    def outbox(chunk):
        pick = (slot_t[:, None, :] == slots[chunk][None, :, None]).astype(jnp.bfloat16)
        sent = jnp.dot(
            pick.reshape(-1, tok_rows), normed, preferred_element_type=jnp.float32
        )
        return sent.astype(jnp.bfloat16).reshape(places, cores, step, -1, LANES)

    def exchanged(blocks):
        return lax.all_to_all(blocks, "sp_0", split_axis=0, concat_axis=0, tiled=True)

    def rowed(block):
        return block.reshape(rows, -1, LANES)

    back = []
    for chunk in range(CHUNKS):
        sent = outbox(chunk)
        came = exchanged(sent)
        other = rowed(came[:, 1])
        other = turned(other, "sp_1", 1)
        here = jnp.concatenate([rowed(came[:, 0]), other], axis=0)
        pieces = [here] + [turned(here, "tp", d) for d in range(1, tp)]
        made = expert_rows(pieces, gate_proj[0], up_proj[0], down_proj[0])
        made = [made[0]] + [turned(made[d], "tp", -d) for d in range(1, tp)]
        sums = made[0].astype(jnp.float32)
        for part in made[1:]:
            sums = sums + part.astype(jnp.float32)
        summed = sums.astype(jnp.bfloat16)
        other = summed[rows:]
        other = turned(other, "sp_1", 1)
        ready = jnp.stack(
            [b.reshape(places, step, -1, LANES) for b in (summed[:rows], other)], axis=1
        )
        came = exchanged(ready)
        back.append(came.reshape(cores * rows, width))

    moe = 0.0
    for k in range(top):
        found = 0.0
        for chunk in range(CHUNKS):
            pick = jnp.where(named[:, k], slot, -1.0)[:, :, None] == slots[chunk]
            found = found + jnp.dot(
                pick.astype(jnp.bfloat16).reshape(tok_rows, -1),
                back[chunk],
                preferred_element_type=jnp.float32,
            )
        moe = moe + found * expert_weights[:, k : k + 1]
    return (stream.astype(jnp.float32) + scaled_norm(moe, post_expert_gain)).astype(jnp.bfloat16)


def solution(mesh):
    split = Mesh(
        mesh.devices.reshape(mesh.shape["grp"], -1, 2, mesh.shape["tp"]),
        GRP_SP_TP,
    )
    tokens = P(GRP_SP_TP, None)
    in_specs = (
        (tokens,) * 4
        + (P(),) * 5
        + (tokens, tokens, P(SP, None, "tp"), P(SP, None, "tp"), P(SP, "tp", None))
    )
    return jax.shard_map(body, mesh=split, in_specs=in_specs, out_specs=tokens, check_vma=False)
```
